32 devices in a mesh: ep: 16 (over z, y, x), tp: 2 (over core).
Axes of the slice: x: 2, y: 2, z: 4, core: 2. Of those that a mesh axis runs over, the one named last changes fastest.
Arguments:
- tokens: bfloat16 [256, 1024], P('ep'), may hold values from -6 to 6
- linear_matrix_state: float32 [256, 16, 4096], P('ep', 'tp'), may hold values from -4 to 4
- mixer_norm_gain: float32 [1024], replicated, may hold values from 0.1 to 1.9
- receptance_weight: bfloat16 [1024, 1024], P(None, 'tp'), may hold values from -0.1875 to 0.1875
- key_weight: bfloat16 [1024, 1024], P(None, 'tp'), may hold values from -0.1875 to 0.1875
- value_weight: bfloat16 [1024, 1024], P(None, 'tp'), may hold values from -0.1875 to 0.1875
- decay_weight: bfloat16 [1024, 1024], P(None, 'tp'), may hold values from -0.1875 to 0.1875
- learning_rate_weight: bfloat16 [1024, 1024], P(None, 'tp'), may hold values from -0.1875 to 0.1875
- output_gate_weight: bfloat16 [1024, 1024], P(None, 'tp'), may hold values from -0.1875 to 0.1875
- decay_offset_bias: float32 [1024], P('tp'), may hold values from -5 to 2
- present_position_factor: float32 [1024], P('tp'), may hold values from -2 to 2
- per_head_gain: float32 [1024], P('tp'), may hold values from 0.1 to 1.9
- head_mix_weight: bfloat16 [1024, 1024], P('tp'), may hold values from -0.1875 to 0.1875
- feedforward_gain: float32 [1024], replicated, may hold values from 0.1 to 1.9
- routing: int32 [256, 2], P('ep'), may hold values from 0 to 15, all different within a row; in each aligned block of 16 rows (0 to 15, 16 to 31, ...) at most 5 rows name the same one
- router_score: float32 [256, 2], P('ep'), may hold values from -6 to 6
- expert_gate_weight: bfloat16 [16, 1024, 1536], P('ep', None, 'tp'), may hold values from -0.1875 to 0.1875
- expert_up_weight: bfloat16 [16, 1024, 1536], P('ep', None, 'tp'), may hold values from -0.1875 to 0.1875
- expert_down_weight: bfloat16 [16, 1536, 1024], P('ep', 'tp'), may hold values from -0.15625 to 0.15625
Outputs:
- layer_out: bfloat16 [256, 1024], P('ep')
- new_state: float32 [256, 16, 4096], P('ep', 'tp')
The draws below stay inside these ranges and needn't reach their ends.
Inputs may be any that keep to these rules, and one draw needn't show every extreme that they name: `routing`: each row names 2 different experts. Among the rows of one index of ep no expert is named more than 5 times, a bound that some block reaches.
All inputs are finite; a program needn't handle non-finite values.
Results may differ from the reference program's by a relative error of at most 0.013.
Values may be sent and summed in bfloat16 or wider, within the bound.
A program may use at most 64 MiB of HBM per device.

```python
import math
import jax
import jax.numpy as jnp
import numpy as np
from jax import lax

D = 1024
HEADS = 16
HEAD = 64
FF = 1536
TOP = 2
SEQ_DEV = 16
TOTAL_CHANNELS = 1024
SEQS = 256
EXPERTS = 16
CAP = 5
N_EP = 16


def level_of(rng, shape, split, smallest, largest):
    level, own = 1.0, jax.random.fold_in(rng, 6)
    for dim, blocks in split:
        steps = jnp.exp(jax.random.uniform(jax.random.fold_in(own, dim), (blocks,), jnp.float32, smallest / len(split), largest / len(split)))
        level = level * jnp.repeat(steps, shape[dim] // blocks).reshape([-1 if axis == dim else 1 for axis in range(len(shape))])
    return level


def routed_block(stream_key, own, number, rows, amount, top, reach, slope):
    order = jax.random.permutation(stream_key, amount)
    crowded, common = portions_of(amount, rows * top, reach, slope, True), portions_of(amount, rows * top, reach, slope, False)
    places = jnp.arange(amount)

    def named(tallies, offset_by):
        used = int((tallies > 0).sum())
        fixed = max(1, used // 4)
        passed = fixed + (places - fixed + offset_by * (used - fixed)) % max(1, amount - fixed)
        return jnp.zeros((amount,), jnp.int32).at[order[jnp.where(places < fixed, places, passed)]].set(jnp.asarray(tallies, jnp.int32))

    tallies = jnp.where(number % 4 == 0, named(crowded, number // 4), named(common, number - number // 4 - 1))
    mixed = jax.random.permutation(jax.random.fold_in(own, 3), amount)
    giver, receiver = mixed[0:amount // 2 * 2:2], mixed[1:amount // 2 * 2:2]
    margin = jnp.minimum(tallies[giver] - 1, reach - tallies[receiver]) // 2
    margin = jnp.where((giver == order[0]) | (receiver == order[0]) | (tallies[receiver] == 0), 0, jnp.maximum(margin, 0))
    passed = jax.random.randint(jax.random.fold_in(own, 4), (amount // 2,), 0, 1 << 20) % (margin + 1)
    tallies = tallies.at[giver].add(-passed).at[receiver].add(passed)
    labels = jnp.searchsorted(jnp.cumsum(tallies), jnp.arange(rows * top), side="right").astype(jnp.int32)
    table = labels.reshape(top, rows).T
    table = table[jax.random.permutation(jax.random.fold_in(own, 1), rows)]
    offset_by = jax.random.randint(jax.random.fold_in(own, 2), (rows, 1), 0, top)
    return jnp.take_along_axis(table, (jnp.arange(top)[None, :] + offset_by) % top, axis=1)


def portions_of(count, total, limit, lean, full):
    portions = [(1 << 20) // math.isqrt(standing ** lean) + 1 for standing in range(1, count + 1)]
    largest = limit if full else min(limit, max(-(-total // count), total * portions[0] // sum(portions)))
    least = 1 if total - largest >= count - 1 else 0
    holding, rest = [largest] + [least] * (count - 1), total - largest - least * (count - 1)
    while rest > 0:
        movable = [i for i in range(1, count) if holding[i] < largest] or [i for i in range(1, count) if holding[i] < limit]
        mass, left = sum([portions[i] for i in movable]), rest
        for i in movable:
            more = min(limit - holding[i], max(1, left * portions[i] // mass), rest)
            holding[i] = holding[i] + more
            rest = rest - more
    return np.array(holding)


def gaussian(rng, extent, deviation, most, split=(), held_as=jnp.bfloat16):
    array = deviation * jax.random.normal(rng, extent, jnp.float32)
    if split:
        array = array * level_of(rng, extent, split, -0.22, 0.18)
    return jnp.clip(array, -most, most).astype(held_as)


def setup_inputs(seed: int = 0) -> dict:
    streams_of = jax.random.split(jax.random.key(seed), 20)
    tokens = gaussian(streams_of[0], (SEQS, D), 1.0, 6.0, ((0, 16),))
    linear_matrix_state = gaussian(streams_of[1], (SEQS, HEADS, HEAD * HEAD), 0.5, 4.0, ((0, 16), (1, 2)), jnp.float32)
    mixer_norm_gain = jnp.clip(1.0 + 0.18 * jax.random.normal(streams_of[2], (D,), jnp.float32), 0.1, 1.9)
    receptance_weight = gaussian(streams_of[3], (D, TOTAL_CHANNELS), D ** -0.5, 0.1875, ((1, 2),))
    key_weight = gaussian(streams_of[4], (D, TOTAL_CHANNELS), D ** -0.5, 0.1875, ((1, 2),))
    value_weight = gaussian(streams_of[5], (D, TOTAL_CHANNELS), D ** -0.5, 0.1875, ((1, 2),))
    decay_weight = gaussian(streams_of[6], (D, TOTAL_CHANNELS), D ** -0.5, 0.1875, ((1, 2),))
    learning_rate_weight = gaussian(streams_of[7], (D, TOTAL_CHANNELS), D ** -0.5, 0.1875, ((1, 2),))
    output_gate_weight = gaussian(streams_of[8], (D, TOTAL_CHANNELS), D ** -0.5, 0.1875, ((1, 2),))
    decay_offset_bias = jnp.clip(-5.0 + 7.0 * jax.random.uniform(streams_of[9], (TOTAL_CHANNELS,), jnp.float32) ** level_of(streams_of[9], (TOTAL_CHANNELS,), ((0, 2),), -0.2, 0.2), -5.0, 2.0)
    present_position_factor = gaussian(streams_of[10], (TOTAL_CHANNELS,), 0.3, 2.0, ((0, 2),), jnp.float32)
    per_head_gain = jnp.clip(1.0 + 0.18 * jax.random.normal(streams_of[11], (TOTAL_CHANNELS,), jnp.float32), 0.1, 1.9)
    head_mix_weight = gaussian(streams_of[12], (TOTAL_CHANNELS, D), TOTAL_CHANNELS ** -0.5, 0.1875, ((0, 2),))
    feedforward_gain = jnp.clip(1.0 + 0.18 * jax.random.normal(streams_of[13], (D,), jnp.float32), 0.1, 1.9)
    routing_keys = jax.random.split(jax.random.fold_in(streams_of[14], 1), SEQS // SEQ_DEV)
    routing_turns = jax.random.permutation(jax.random.fold_in(streams_of[14], 3), SEQS // SEQ_DEV)
    routing = jax.vmap(lambda own, number: routed_block(jax.random.fold_in(streams_of[14], 2), own, number, SEQ_DEV, EXPERTS, TOP, CAP, 2))(routing_keys, routing_turns).reshape((SEQS, TOP))
    router_score = gaussian(streams_of[15], (SEQS, TOP), 1.5, 6.0, ((0, 16),), jnp.float32)
    expert_gate_weight = gaussian(streams_of[16], (EXPERTS, D, FF), D ** -0.5, 0.1875, ((0, 16), (2, 2)))
    expert_up_weight = gaussian(streams_of[17], (EXPERTS, D, FF), D ** -0.5, 0.1875, ((0, 16), (2, 2)))
    expert_down_weight = gaussian(streams_of[18], (EXPERTS, FF, D), FF ** -0.5, 0.15625, ((0, 16), (1, 2)))
    return dict(tokens=tokens, linear_matrix_state=linear_matrix_state, mixer_norm_gain=mixer_norm_gain, receptance_weight=receptance_weight, key_weight=key_weight, value_weight=value_weight, decay_weight=decay_weight, learning_rate_weight=learning_rate_weight, output_gate_weight=output_gate_weight, decay_offset_bias=decay_offset_bias, present_position_factor=present_position_factor, per_head_gain=per_head_gain, head_mix_weight=head_mix_weight, feedforward_gain=feedforward_gain, routing=routing, router_score=router_score, expert_gate_weight=expert_gate_weight, expert_up_weight=expert_up_weight, expert_down_weight=expert_down_weight)


NORM_EPS = 1e-06
UNIT_EPS = 1e-05
HEAD_EPS = 0.00064

def rms_scale(values, gain):
    values = values.astype(jnp.float32)
    factor = lax.rsqrt(lax.optimization_barrier(jnp.mean(values * values, axis=-1, keepdims=True)) + NORM_EPS)
    return values * factor * gain

def project(normalized_input, weight):
    return jnp.dot(normalized_input, weight, preferred_element_type=jnp.float32)

def mixer_head_rows(normalized_input, linear_matrix_state, receptance_weight, key_weight, value_weight, decay_weight, learning_rate_weight, output_gate_weight, decay_offset_bias, present_position_factor, per_head_gain):
    batch_length = normalized_input.shape[0]
    head_count = linear_matrix_state.shape[1]
    head_width = key_weight.shape[1] // head_count
    shape = (batch_length, head_count, head_width)
    receptance = project(normalized_input, receptance_weight).reshape(shape)
    key = project(normalized_input, key_weight).reshape(shape)
    value = project(normalized_input, value_weight).reshape(shape)
    log_rate = -jax.nn.softplus(-(decay_offset_bias + project(normalized_input, decay_weight))) - 0.5
    decay = jnp.exp(-jnp.exp(log_rate)).reshape(shape)
    rate = jax.nn.sigmoid(project(normalized_input, learning_rate_weight)).reshape(shape)
    gating = jax.nn.sigmoid(project(normalized_input, output_gate_weight))
    unit = key * lax.rsqrt(lax.optimization_barrier(jnp.sum(key * key, axis=-1, keepdims=True)) + UNIT_EPS)
    shifted_key = key * rate
    matrix = linear_matrix_state.reshape(batch_length, head_count, head_width, head_width)
    removed = lax.optimization_barrier(jnp.sum(matrix * unit[:, :, None, :], axis=-1))
    updated = matrix * decay[:, :, None, :] - removed[..., None] * (unit * rate)[:, :, None, :] + value[..., None] * shifted_key[:, :, None, :]
    read = lax.optimization_barrier(jnp.sum(updated * receptance[:, :, None, :], axis=-1))
    center = read - lax.optimization_barrier(jnp.mean(read, axis=-1, keepdims=True))
    scaled = center * lax.rsqrt(lax.optimization_barrier(jnp.mean(center * center, axis=-1, keepdims=True)) + HEAD_EPS)
    scaled = scaled * per_head_gain.reshape(head_count, head_width)
    own_term = lax.optimization_barrier(jnp.sum(receptance * shifted_key * present_position_factor.reshape(head_count, head_width), axis=-1, keepdims=True)) * value
    merged = ((scaled + own_term).reshape(batch_length, head_count * head_width) * gating).astype(jnp.bfloat16)
    return (merged, updated.reshape(batch_length, head_count, head_width * head_width))

def reference(tokens, linear_matrix_state, mixer_norm_gain, receptance_weight, key_weight, value_weight, decay_weight, learning_rate_weight, output_gate_weight, decay_offset_bias, present_position_factor, per_head_gain, head_mix_weight, feedforward_gain, routing, router_score, expert_gate_weight, expert_up_weight, expert_down_weight):
    normalized_input = rms_scale(tokens, mixer_norm_gain).astype(jnp.bfloat16)

    def block_mixer(pieces):
        return mixer_head_rows(pieces[0], pieces[1], receptance_weight, key_weight, value_weight, decay_weight, learning_rate_weight, output_gate_weight, decay_offset_bias, present_position_factor, per_head_gain)
    merged, new_state = lax.map(block_mixer, (normalized_input.reshape(N_EP, SEQ_DEV, D), linear_matrix_state.reshape(N_EP, SEQ_DEV, HEADS, HEAD * HEAD)))
    merged = merged.reshape(SEQS, TOTAL_CHANNELS)
    new_state = new_state.reshape(SEQS, HEADS, HEAD * HEAD)
    mix = jnp.dot(merged, head_mix_weight, preferred_element_type=jnp.float32).astype(jnp.bfloat16)
    residual = tokens.astype(jnp.float32) + mix.astype(jnp.float32)
    expert_in = rms_scale(residual, feedforward_gain).astype(jnp.bfloat16)
    first = jax.nn.sigmoid(router_score[:, 0] - router_score[:, 1])
    second = jax.nn.sigmoid(router_score[:, 1] - router_score[:, 0])
    weights = jnp.stack([first, second], axis=1)
    slot_count = N_EP * CAP
    flat_route = routing.reshape(-1)

    def one_expert(expert):
        chosen = flat_route == expert
        picked = jnp.nonzero(chosen, size=slot_count, fill_value=0)[0].astype(jnp.int32)
        live = jnp.arange(slot_count, dtype=jnp.int32) < jnp.sum(chosen.astype(jnp.int32))
        inputs = expert_in[picked // TOP]
        gate_in = jnp.dot(inputs, expert_gate_weight[expert], preferred_element_type=jnp.float32)
        up_in = jnp.dot(inputs, expert_up_weight[expert], preferred_element_type=jnp.float32)
        hidden = (jax.nn.silu(gate_in) * up_in).astype(jnp.bfloat16)
        result = jnp.dot(hidden, expert_down_weight[expert], preferred_element_type=jnp.float32).astype(jnp.bfloat16)
        return (jnp.where(live[:, None], result.astype(jnp.float32), jnp.float32(0.0)), picked)
    results, picks = lax.map(one_expert, jnp.arange(EXPERTS, dtype=jnp.int32))
    gathered = jnp.zeros((SEQS * TOP, D), jnp.float32).at[picks.reshape(-1)].add(results.reshape(-1, D))
    routed = gathered.reshape(SEQS, TOP, D)
    layer_out = (residual + lax.optimization_barrier(jnp.sum(weights[:, :, None] * routed, axis=1))).astype(jnp.bfloat16)
    return (layer_out, new_state)
```

```python
import functools
import math

import jax
import jax.numpy as jnp
from jax import lax
from jax.experimental import pallas as pl
from jax.experimental.pallas import tpu as pltpu
from jax.sharding import PartitionSpec as P

NORM_EPS = 1e-06
UNIT_EPS = 1e-05
HEAD_EPS = 0.00064
LANES = 128
F32 = jnp.float32
BF16 = jnp.bfloat16
HBM = pl.BlockSpec(memory_space=pl.ANY)
VMEM = pl.BlockSpec(memory_space=pltpu.VMEM)
MESH = pl.DeviceIdType.MESH
DECAY_SCALE = math.exp(-0.5)


def dot(a, b):
    return jnp.dot(a, b, preferred_element_type=F32)


def rms_scale(values, gain):
    factor = lax.rsqrt(jnp.mean(values * values, axis=-1, keepdims=True) + NORM_EPS)
    return values * factor * gain


def split(x):
    high = x.astype(BF16)
    return high, (x - high.astype(F32)).astype(BF16)


def to_head_rows(x, ref, heads):
    seqs = x.shape[0]
    low = lax.broadcasted_iota(jnp.int32, (seqs, LANES), 1) < LANES // 2
    for pair in range(heads // 2):
        here = x[:, pair * LANES : (pair + 1) * LANES]
        turned = pltpu.roll(here, LANES // 2, 1)
        ref[pl.ds(2 * pair, seqs, stride=heads), :] = jnp.where(low, here, turned)
        ref[pl.ds(2 * pair + 1, seqs, stride=heads), :] = jnp.where(low, turned, here)


def from_head_rows(ref, seqs, heads):
    low = lax.broadcasted_iota(jnp.int32, (seqs, LANES), 1) < LANES // 2
    parts = []
    for pair in range(heads // 2):
        even = ref[pl.ds(2 * pair, seqs, stride=heads), :]
        odd = ref[pl.ds(2 * pair + 1, seqs, stride=heads), :]
        parts.append(jnp.where(low, even, odd))
    return jnp.concatenate(parts, axis=1)


def mixer_kernel(
    tokens_ref,
    state_hbm,
    norm_gain_ref,
    wr_hbm,
    wk_hbm,
    wv_hbm,
    wd_hbm,
    wl_hbm,
    wg_hbm,
    bias_ref,
    factor_ref,
    head_gain_ref,
    wm_hbm,
    partial_ref,
    new_hbm,
    state,
    wr,
    wk,
    wv,
    wd,
    wl,
    wg,
    wm,
    r_rows,
    k_rows,
    v_rows,
    d_rows,
    l_rows,
    f_rows,
    g_rows,
    o_rows,
    products,
    gatherer,
    sems,
    out_sems,
):
    seqs, heads, cells = state.shape
    rows = seqs * heads
    width = LANES // 2
    sources = [wk_hbm, wr_hbm, wd_hbm, wl_hbm, state_hbm, wv_hbm, wg_hbm, wm_hbm]
    targets = [wk, wr, wd, wl, state, wv, wg, wm]
    copies = [
        pltpu.make_async_copy(a, b, sems.at[i]) for i, (a, b) in enumerate(zip(sources, targets))
    ]
    for copy in copies:
        copy.start()

    normed = rms_scale(tokens_ref[...].astype(F32), norm_gain_ref[...]).astype(BF16)
    channels = heads * width
    to_head_rows(jnp.broadcast_to(factor_ref[...], (seqs, channels)), f_rows, heads)
    to_head_rows(jnp.broadcast_to(head_gain_ref[...], (seqs, channels)), g_rows, heads)
    chunk = 512
    for c in range(cells // chunk):
        at = lax.broadcasted_iota(jnp.int32, (chunk, LANES), 0) // width
        to = lax.broadcasted_iota(jnp.int32, (chunk, LANES), 1) % width
        gatherer[pl.ds(c * chunk, chunk), :] = jnp.where(
            to - at == c * (chunk // width), 1.0, 0.0
        ).astype(BF16)

    copies[0].wait()
    to_head_rows(dot(normed, wk[...]), k_rows, heads)
    copies[1].wait()
    to_head_rows(dot(normed, wr[...]), r_rows, heads)
    copies[2].wait()
    decay_in = dot(normed, wd[...]) + bias_ref[...]
    to_head_rows(jnp.exp(-DECAY_SCALE * jax.nn.sigmoid(decay_in)), d_rows, heads)
    copies[3].wait()
    to_head_rows(jax.nn.sigmoid(dot(normed, wl[...])), l_rows, heads)

    key = k_rows[...]
    unit = key * lax.rsqrt(jnp.sum(key * key, axis=-1, keepdims=True) * 0.5 + UNIT_EPS)
    decay = d_rows[...]
    rate = l_rows[...]
    receptance = r_rows[...]
    shifted = key * rate
    unit_rate = unit * rate
    decay_receptance = decay * receptance

    copies[4].wait()
    for c in range(cells // LANES):
        lanes = pl.ds(c * LANES, LANES)
        x = state[:, :, lanes].reshape(rows, LANES)
        products[0:rows, lanes] = (x * unit).astype(BF16)
        high, low = split(x * decay_receptance)
        products[rows : 2 * rows, lanes] = high
        products[2 * rows : 3 * rows, lanes] = low
    copies[5].wait()
    to_head_rows(dot(normed, wv[...]), v_rows, heads)
    value = v_rows[...]
    sums = dot(products[...], gatherer[...])
    removed = sums[0:rows]
    read = sums[rows : 2 * rows] + sums[2 * rows :]

    def head_sum(x):
        return jnp.sum(x, axis=-1, keepdims=True) * 0.5

    read = read - removed * head_sum(unit_rate * receptance) + value * head_sum(shifted * receptance)
    center = read - head_sum(read) * (1.0 / width)
    scaled = center * lax.rsqrt(head_sum(center * center) * (1.0 / width) + HEAD_EPS)
    own = head_sum(receptance * shifted * f_rows[...])
    o_rows[...] = scaled * g_rows[...] + own * value
    copies[6].wait()
    gating = jax.nn.sigmoid(dot(normed, wg[...]))
    merged = (from_head_rows(o_rows, seqs, heads) * gating).astype(BF16)
    copies[7].wait()
    partial_ref[...] = dot(merged, wm[...]).astype(BF16)

    first = lax.broadcasted_iota(jnp.int32, (rows, LANES), 1) < width
    v_high, v_low = split(value)
    m_high, m_low = split(removed)
    compact = jnp.concatenate(
        [
            jnp.where(first, v_high.astype(F32), v_low.astype(F32)).astype(BF16),
            jnp.where(first, m_high.astype(F32), m_low.astype(F32)).astype(BF16),
        ],
        axis=0,
    )
    writes = []
    for c in range(cells // chunk):
        spread = lax.dot_general(
            compact,
            gatherer[pl.ds(c * chunk, chunk), :],
            (((1,), (1,)), ((), ())),
            preferred_element_type=F32,
        )
        for b in range(chunk // LANES):
            lanes = pl.ds(c * chunk + b * LANES, LANES)
            x = state[:, :, lanes].reshape(rows, LANES)
            v_here = spread[0:rows, b * LANES : (b + 1) * LANES]
            m_here = spread[rows:, b * LANES : (b + 1) * LANES]
            new = x * decay + v_here * shifted - m_here * unit_rate
            state[:, :, lanes] = new.reshape(seqs, heads, LANES)
        part = pl.ds(c * chunk, chunk)
        write = pltpu.make_async_copy(
            state.at[:, :, part], new_hbm.at[:, :, part], out_sems.at[c]
        )
        write.start()
        writes.append(write)
    for write in writes:
        write.wait()


def expert_kernel(
    experts,
    capacity,
    tokens_ref,
    partial_ref,
    gain_ref,
    routing_ref,
    score_ref,
    gate_hbm,
    up_hbm,
    down_hbm,
    out_ref,
    wg,
    wu,
    wd,
    other_partial,
    features,
    outgoing,
    arrived,
    paired,
    crossing,
    crossed,
    results,
    returned,
    final,
    w_sems,
    pair_send,
    pair_recv,
    go_send,
    go_recv,
    fwd_send,
    fwd_recv,
    back_send,
    back_recv,
    local_sems,
):
    me = lax.axis_index("ep")
    side = lax.axis_index("tp")
    other = 1 - side
    seqs, model = tokens_ref.shape
    half = model // 2
    rows = experts * capacity

    barrier = pltpu.get_barrier_semaphore()
    pl.semaphore_signal(barrier, inc=1, device_id=(me, other), device_id_type=MESH)

    @pl.loop(1, experts)
    def _(k):
        pl.semaphore_signal(
            barrier, inc=1, device_id=(lax.rem(me + k, experts), side), device_id_type=MESH
        )

    loads = [
        pltpu.make_async_copy(a.at[0], b, w_sems.at[i])
        for i, (a, b) in enumerate([(gate_hbm, wg), (up_hbm, wu), (down_hbm, wd)])
    ]
    for load in loads:
        load.start()

    route0 = routing_ref[:, 0:1]
    route1 = routing_ref[:, 1:2]
    names = lax.broadcasted_iota(jnp.int32, (seqs, experts), 1)
    hot0 = jnp.where(route0 == names, 1.0, 0.0)
    hot1 = jnp.where(route1 == names, 1.0, 0.0)
    below = jnp.where(
        lax.broadcasted_iota(jnp.int32, (seqs, seqs), 1)
        < lax.broadcasted_iota(jnp.int32, (seqs, seqs), 0),
        1.0,
        0.0,
    ).astype(BF16)
    before0 = dot(below, hot0.astype(BF16))
    before1 = dot(below, hot1.astype(BF16)) + jnp.sum(hot0, axis=0, keepdims=True)
    slot0 = jnp.sum(before0 * hot0, axis=1, keepdims=True).astype(jnp.int32)
    slot1 = jnp.sum(before1 * hot1, axis=1, keepdims=True).astype(jnp.int32)
    spots = lax.broadcasted_iota(jnp.int32, (seqs, rows), 1)
    place0 = jnp.where(route0 * capacity + slot0 == spots, 1.0, 0.0)
    place1 = jnp.where(route1 * capacity + slot1 == spots, 1.0, 0.0)
    placed = (place0 + place1).astype(BF16)
    place0 = place0.astype(BF16)
    place1 = place1.astype(BF16)
    difference = score_ref[:, 0:1] - score_ref[:, 1:2]
    weight0 = jax.nn.sigmoid(difference)
    weight1 = jax.nn.sigmoid(-difference)

    pl.semaphore_wait(barrier, experts)

    def to_pair(source, target, index):
        return pltpu.make_async_remote_copy(
            src_ref=source,
            dst_ref=target,
            send_sem=pair_send.at[index],
            recv_sem=pair_recv.at[index],
            device_id=(me, other),
            device_id_type=MESH,
        )

    mix_copy = to_pair(partial_ref, other_partial, 0)
    mix_copy.start()
    mix_copy.wait()
    mix = (partial_ref[...].astype(F32) + other_partial[...].astype(F32)).astype(BF16)
    residual = tokens_ref[...].astype(F32) + mix.astype(F32)
    expert_in = rms_scale(residual, gain_ref[...])
    own_lanes = pl.ds(pl.multiple_of(side * half, LANES), half)
    other_lanes = pl.ds(pl.multiple_of(other * half, LANES), half)
    mine = jnp.where(side == 0, expert_in[:, :half], expert_in[:, half:]).astype(BF16)
    own_residual = jnp.where(side == 0, residual[:, :half], residual[:, half:])
    packed = lax.dot_general(
        placed, mine, (((0,), (0,)), ((), ())), preferred_element_type=F32
    )
    outgoing[...] = packed.reshape(experts, capacity, half).astype(BF16)

    def go(k):
        peer = lax.rem(me + k, experts)
        return pltpu.make_async_remote_copy(
            src_ref=outgoing.at[peer],
            dst_ref=arrived.at[me],
            send_sem=go_send.at[k],
            recv_sem=go_recv.at[k],
            device_id=(peer, side),
            device_id_type=MESH,
        )

    def forward(k):
        source = lax.rem(me - k + experts, experts)
        return pltpu.make_async_remote_copy(
            src_ref=arrived.at[source],
            dst_ref=paired.at[source],
            send_sem=fwd_send.at[k],
            recv_sem=fwd_recv.at[k],
            device_id=(me, other),
            device_id_type=MESH,
        )

    @pl.loop(1, experts)
    def _(k):
        go(k).start()

    keep = pltpu.make_async_copy(outgoing.at[me], arrived.at[me], local_sems.at[0])
    keep.start()
    keep.wait()
    forward(0).start()

    @pl.loop(1, experts)
    def _(k):
        go(k).wait_recv()
        forward(k).start()

    own_rows = pl.ds(pl.multiple_of(side * half, LANES), half)
    other_rows = pl.ds(pl.multiple_of(other * half, LANES), half)
    x = arrived[...].astype(F32).reshape(rows, half).astype(BF16)
    loads[0].wait()
    loads[1].wait()
    gate = dot(x, wg[own_rows, :])
    up = dot(x, wu[own_rows, :])

    @pl.loop(0, experts)
    def _(k):
        forward(k).wait_recv()

    x = paired[...].astype(F32).reshape(rows, half).astype(BF16)
    gate = gate + dot(x, wg[other_rows, :])
    up = up + dot(x, wu[other_rows, :])
    hidden = (jax.nn.silu(gate) * up).astype(BF16)
    loads[2].wait()
    crossing[...] = dot(hidden, wd[:, other_lanes]).astype(BF16)
    cross_copy = to_pair(crossing, crossed, 1)
    cross_copy.start()
    own_result = dot(hidden, wd[:, own_lanes])
    cross_copy.wait()
    own_result = own_result + crossed[...].astype(F32)
    results[...] = own_result.reshape(experts, capacity, half).astype(BF16)

    def back(k):
        peer = lax.rem(me + k, experts)
        return pltpu.make_async_remote_copy(
            src_ref=results.at[peer],
            dst_ref=returned.at[me],
            send_sem=back_send.at[k],
            recv_sem=back_recv.at[k],
            device_id=(peer, side),
            device_id_type=MESH,
        )

    @pl.loop(1, experts)
    def _(k):
        back(k).start()

    keep = pltpu.make_async_copy(results.at[me], returned.at[me], local_sems.at[1])
    keep.start()
    keep.wait()

    @pl.loop(1, experts)
    def _(k):
        back(k).wait_recv()

    y = returned[...].astype(F32).reshape(rows, half).astype(BF16)
    final[...] = (own_residual + weight0 * dot(place0, y) + weight1 * dot(place1, y)).astype(BF16)
    final_copy = to_pair(final, out_ref.at[:, own_lanes], 2)
    final_copy.start()
    out_ref[:, own_lanes] = final[...]
    final_copy.wait()

    forward(0).wait_send()

    @pl.loop(1, experts)
    def _(k):
        go(k).wait_send()
        forward(k).wait_send()
        back(k).wait_send()


def body(
    tokens,
    linear_matrix_state,
    mixer_norm_gain,
    receptance_weight,
    key_weight,
    value_weight,
    decay_weight,
    learning_rate_weight,
    output_gate_weight,
    decay_offset_bias,
    present_position_factor,
    per_head_gain,
    head_mix_weight,
    feedforward_gain,
    routing,
    router_score,
    expert_gate_weight,
    expert_up_weight,
    expert_down_weight,
):
    seqs, model = tokens.shape
    _, heads, cells = linear_matrix_state.shape
    rows = seqs * heads
    weights = (
        receptance_weight,
        key_weight,
        value_weight,
        decay_weight,
        learning_rate_weight,
        output_gate_weight,
    )
    head_rows = pltpu.VMEM((rows, LANES), F32)
    partial, new_state = pl.pallas_call(
        mixer_kernel,
        out_shape=(
            jax.ShapeDtypeStruct((seqs, model), BF16),
            jax.ShapeDtypeStruct(linear_matrix_state.shape, F32),
        ),
        in_specs=[VMEM, HBM, VMEM] + [HBM] * 6 + [VMEM] * 3 + [HBM],
        out_specs=(VMEM, HBM),
        scratch_shapes=[pltpu.VMEM(linear_matrix_state.shape, F32)]
        + [pltpu.VMEM(w.shape, BF16) for w in weights]
        + [pltpu.VMEM(head_mix_weight.shape, BF16)]
        + [head_rows] * 8
        + [
            pltpu.VMEM((3 * rows, cells), BF16),
            pltpu.VMEM((cells, LANES), BF16),
            pltpu.SemaphoreType.DMA((8,)),
            pltpu.SemaphoreType.DMA((cells // 512,)),
        ],
        name="mixer",
    )(
        tokens,
        linear_matrix_state,
        mixer_norm_gain.reshape(1, -1),
        *weights,
        decay_offset_bias.reshape(1, -1),
        present_position_factor.reshape(1, -1),
        per_head_gain.reshape(1, -1),
        head_mix_weight,
    )

    experts = lax.axis_size("ep")
    capacity = max(2, 8 * seqs * routing.shape[1] // (3 * experts))
    capacity = -(-capacity // 8) * 8
    half = model // 2
    exchange = pltpu.VMEM((experts, capacity, half), BF16)
    layer_out = pl.pallas_call(
        functools.partial(expert_kernel, experts, capacity),
        out_shape=jax.ShapeDtypeStruct((seqs, model), BF16),
        in_specs=[VMEM] * 5 + [HBM] * 3,
        out_specs=VMEM,
        scratch_shapes=[
            pltpu.VMEM(expert_gate_weight.shape[1:], BF16),
            pltpu.VMEM(expert_up_weight.shape[1:], BF16),
            pltpu.VMEM(expert_down_weight.shape[1:], BF16),
            pltpu.VMEM((seqs, model), BF16),
            pltpu.VMEM((seqs, model), BF16),
            exchange,
            exchange,
            exchange,
            pltpu.VMEM((experts * capacity, half), BF16),
            pltpu.VMEM((experts * capacity, half), BF16),
            exchange,
            exchange,
            pltpu.VMEM((seqs, half), BF16),
            pltpu.SemaphoreType.DMA((3,)),
            pltpu.SemaphoreType.DMA((3,)),
            pltpu.SemaphoreType.DMA((3,)),
        ]
        + [pltpu.SemaphoreType.DMA((experts,))] * 6
        + [pltpu.SemaphoreType.DMA((2,))],
        compiler_params=pltpu.CompilerParams(collective_id=0, has_side_effects=True),
        name="experts",
    )(
        tokens,
        partial,
        feedforward_gain.reshape(1, -1),
        routing,
        router_score,
        expert_gate_weight,
        expert_up_weight,
        expert_down_weight,
    )
    return (layer_out, new_state)


def solution(mesh):
    return jax.shard_map(
        body,
        mesh=mesh,
        in_specs=(
            P("ep", None),
            P("ep", "tp", None),
            P(),
            P(None, "tp"),
            P(None, "tp"),
            P(None, "tp"),
            P(None, "tp"),
            P(None, "tp"),
            P(None, "tp"),
            P("tp"),
            P("tp"),
            P("tp"),
            P("tp", None),
            P(),
            P("ep", None),
            P("ep", None),
            P("ep", None, "tp"),
            P("ep", None, "tp"),
            P("ep", "tp", None),
        ),
        out_specs=(P("ep", None), P("ep", "tp", None)),
        check_vma=False,
    )
```

```python
import functools
import math

import jax
import jax.numpy as jnp
from jax import lax
from jax.experimental import pallas as pl
from jax.experimental.pallas import tpu as pltpu
from jax.sharding import PartitionSpec as P

NORM_EPS = 1e-06
UNIT_EPS = 1e-05
HEAD_EPS = 0.00064
LANES = 128
F32 = jnp.float32
BF16 = jnp.bfloat16
HBM = pl.BlockSpec(memory_space=pl.ANY)
VMEM = pl.BlockSpec(memory_space=pltpu.VMEM)
MESH = pl.DeviceIdType.MESH
DECAY_SCALE = math.exp(-0.5)


def dot(a, b):
    return jnp.dot(a, b, preferred_element_type=F32)


def rms_scale(values, gain):
    factor = lax.rsqrt(jnp.mean(values * values, axis=-1, keepdims=True) + NORM_EPS)
    return values * factor * gain


def split(x):
    high = x.astype(BF16)
    return high, (x - high.astype(F32)).astype(BF16)


def to_head_rows(x, ref, heads):
    seqs = x.shape[0]
    low = lax.broadcasted_iota(jnp.int32, (seqs, LANES), 1) < LANES // 2
    for pair in range(heads // 2):
        here = x[:, pair * LANES : (pair + 1) * LANES]
        turned = pltpu.roll(here, LANES // 2, 1)
        ref[pl.ds(2 * pair, seqs, stride=heads), :] = jnp.where(low, here, turned)
        ref[pl.ds(2 * pair + 1, seqs, stride=heads), :] = jnp.where(low, turned, here)


def from_head_rows(ref, seqs, heads):
    low = lax.broadcasted_iota(jnp.int32, (seqs, LANES), 1) < LANES // 2
    parts = []
    for pair in range(heads // 2):
        even = ref[pl.ds(2 * pair, seqs, stride=heads), :]
        odd = ref[pl.ds(2 * pair + 1, seqs, stride=heads), :]
        parts.append(jnp.where(low, even, odd))
    return jnp.concatenate(parts, axis=1)


def layer_kernel(
    experts,
    capacity,
    sent,
    tokens_ref,
    state_hbm,
    norm_gain_ref,
    wr_hbm,
    wk_hbm,
    wv_hbm,
    wd_hbm,
    wl_hbm,
    wg_hbm,
    bias_ref,
    factor_ref,
    head_gain_ref,
    wm_hbm,
    gain_ref,
    routing_ref,
    score_ref,
    gate_hbm,
    up_hbm,
    down_hbm,
    out_ref,
    state,
    wr,
    wk,
    wv,
    wd,
    wl,
    wg,
    wm,
    r_rows,
    k_rows,
    v_rows,
    d_rows,
    l_rows,
    f_rows,
    g_rows,
    o_rows,
    products,
    gatherer,
    e_gate,
    e_up,
    e_down,
    own_partial,
    other_partial,
    outgoing,
    arrived,
    paired,
    crossing,
    crossed,
    results,
    returned,
    final,
    sems,
    pair_send,
    pair_recv,
    go_send,
    go_recv,
    fwd_send,
    fwd_recv,
    back_send,
    back_recv,
    local_sems,
):
    me = lax.axis_index("ep")
    side = lax.axis_index("tp")
    other = 1 - side
    seqs, heads, cells = state.shape
    rows = seqs * heads
    width = LANES // 2
    model = tokens_ref.shape[1]
    half = model // 2
    places = experts * capacity

    sources = [wk_hbm, wr_hbm, wd_hbm, wl_hbm, state_hbm, wv_hbm, wg_hbm, wm_hbm]
    targets = [wk, wr, wd, wl, state, wv, wg, wm]
    sources += [gate_hbm.at[0], up_hbm.at[0], down_hbm.at[0]]
    targets += [e_gate, e_up, e_down]
    copies = [
        pltpu.make_async_copy(a, b, sems.at[i]) for i, (a, b) in enumerate(zip(sources, targets))
    ]
    for copy in copies:
        copy.start()

    blank = jnp.zeros(arrived.shape, BF16)
    arrived[...] = blank
    paired[...] = blank
    returned[...] = blank

    barrier = pltpu.get_barrier_semaphore()
    pl.semaphore_signal(barrier, inc=1, device_id=(me, other), device_id_type=MESH)

    @pl.loop(1, experts)
    def _(k):
        pl.semaphore_signal(
            barrier, inc=1, device_id=(lax.rem(me + k, experts), side), device_id_type=MESH
        )

    normed = rms_scale(tokens_ref[...].astype(F32), norm_gain_ref[...]).astype(BF16)
    channels = heads * width
    to_head_rows(jnp.broadcast_to(factor_ref[...], (seqs, channels)), f_rows, heads)
    to_head_rows(jnp.broadcast_to(head_gain_ref[...], (seqs, channels)), g_rows, heads)
    chunk = 512
    for c in range(cells // chunk):
        at = lax.broadcasted_iota(jnp.int32, (chunk, LANES), 0) // width
        to = lax.broadcasted_iota(jnp.int32, (chunk, LANES), 1) % width
        gatherer[pl.ds(c * chunk, chunk), :] = jnp.where(
            to - at == c * (chunk // width), 1.0, 0.0
        ).astype(BF16)

    route0 = routing_ref[0:1, :]
    route1 = routing_ref[1:2, :]
    names = lax.broadcasted_iota(jnp.int32, (experts, seqs), 0)
    hot0 = jnp.where(route0 == names, 1.0, 0.0)
    hot1 = jnp.where(route1 == names, 1.0, 0.0)
    row = lax.broadcasted_iota(jnp.int32, (seqs, seqs), 0)
    column = lax.broadcasted_iota(jnp.int32, (seqs, seqs), 1)
    above = jnp.where(row < column, 1.0, 0.0).astype(BF16)
    before0 = dot(hot0.astype(BF16), above)
    before1 = dot(hot1.astype(BF16), above) + jnp.sum(hot0, axis=1, keepdims=True)
    slot0 = jnp.sum(before0 * hot0, axis=0, keepdims=True).astype(jnp.int32)
    slot1 = jnp.sum(before1 * hot1, axis=0, keepdims=True).astype(jnp.int32)
    spots = lax.broadcasted_iota(jnp.int32, (places, seqs), 0)
    place0 = jnp.where(route0 * capacity + slot0 == spots, 1.0, 0.0)
    place1 = jnp.where(route1 * capacity + slot1 == spots, 1.0, 0.0)
    placed = (place0 + place1).astype(BF16)
    place0 = place0.astype(BF16)
    place1 = place1.astype(BF16)
    difference = score_ref[0:1, :] - score_ref[1:2, :]
    difference = jnp.sum(jnp.where(row == column, difference, 0.0), axis=1, keepdims=True)
    weight0 = jax.nn.sigmoid(difference)
    weight1 = jax.nn.sigmoid(-difference)

    copies[0].wait()
    to_head_rows(dot(normed, wk[...]), k_rows, heads)
    copies[1].wait()
    to_head_rows(dot(normed, wr[...]), r_rows, heads)
    copies[2].wait()
    decay_in = dot(normed, wd[...]) + bias_ref[...]
    to_head_rows(jnp.exp(-DECAY_SCALE * jax.nn.sigmoid(decay_in)), d_rows, heads)
    copies[3].wait()
    to_head_rows(jax.nn.sigmoid(dot(normed, wl[...])), l_rows, heads)

    key = k_rows[...]
    unit = key * lax.rsqrt(jnp.sum(key * key, axis=-1, keepdims=True) * 0.5 + UNIT_EPS)
    decay = d_rows[...]
    rate = l_rows[...]
    receptance = r_rows[...]
    shifted = key * rate
    unit_rate = unit * rate
    decay_receptance = decay * receptance

    copies[4].wait()
    for c in range(cells // LANES):
        lanes = pl.ds(c * LANES, LANES)
        x = state[:, :, lanes].reshape(rows, LANES)
        products[0:rows, lanes] = (x * unit).astype(BF16)
        high, low = split(x * decay_receptance)
        products[rows : 2 * rows, lanes] = high
        products[2 * rows : 3 * rows, lanes] = low
    copies[5].wait()
    to_head_rows(dot(normed, wv[...]), v_rows, heads)
    value = v_rows[...]
    sums = dot(products[...], gatherer[...])
    removed = sums[0:rows]
    read = sums[rows : 2 * rows] + sums[2 * rows :]

    def head_sum(x):
        return jnp.sum(x, axis=-1, keepdims=True) * 0.5

    read = read - removed * head_sum(unit_rate * receptance) + value * head_sum(shifted * receptance)
    center = read - head_sum(read) * (1.0 / width)
    scaled = center * lax.rsqrt(head_sum(center * center) * (1.0 / width) + HEAD_EPS)
    own = head_sum(receptance * shifted * f_rows[...])
    o_rows[...] = scaled * g_rows[...] + own * value
    copies[6].wait()
    gating = jax.nn.sigmoid(dot(normed, wg[...]))
    merged = (from_head_rows(o_rows, seqs, heads) * gating).astype(BF16)
    copies[7].wait()
    own_partial[...] = dot(merged, wm[...]).astype(BF16)
    pl.semaphore_wait(barrier, experts)

    def to_pair(source, target, index):
        return pltpu.make_async_remote_copy(
            src_ref=source,
            dst_ref=target,
            send_sem=pair_send.at[index],
            recv_sem=pair_recv.at[index],
            device_id=(me, other),
            device_id_type=MESH,
        )

    mix_copy = to_pair(own_partial, other_partial, 0)
    mix_copy.start()
    first = lax.broadcasted_iota(jnp.int32, (rows, LANES), 1) < width
    v_high, v_low = split(value)
    m_high, m_low = split(removed)
    compact = jnp.concatenate(
        [
            jnp.where(first, v_high.astype(F32), v_low.astype(F32)).astype(BF16),
            jnp.where(first, m_high.astype(F32), m_low.astype(F32)).astype(BF16),
        ],
        axis=0,
    )

    def update_state(c):
        spread = lax.dot_general(
            compact,
            gatherer[pl.ds(c * chunk, chunk), :],
            (((1,), (1,)), ((), ())),
            preferred_element_type=F32,
        )
        for b in range(chunk // LANES):
            lanes = pl.ds(c * chunk + b * LANES, LANES)
            x = state[:, :, lanes].reshape(rows, LANES)
            v_here = spread[0:rows, b * LANES : (b + 1) * LANES]
            m_here = spread[rows:, b * LANES : (b + 1) * LANES]
            new = x * decay + v_here * shifted - m_here * unit_rate
            state[:, :, lanes] = new.reshape(seqs, heads, LANES)

    mix_copy.wait()
    mix = (own_partial[...].astype(F32) + other_partial[...].astype(F32)).astype(BF16)
    residual = tokens_ref[...].astype(F32) + mix.astype(F32)
    expert_in = rms_scale(residual, gain_ref[...])
    own_part = pl.ds(pl.multiple_of(side * half, LANES), half)
    other_part = pl.ds(pl.multiple_of(other * half, LANES), half)
    mine = jnp.where(side == 0, expert_in[:, :half], expert_in[:, half:]).astype(BF16)
    own_residual = jnp.where(side == 0, residual[:, :half], residual[:, half:])
    outgoing[...] = dot(placed, mine).reshape(experts, capacity, half).astype(BF16)
    used = pl.ds(0, sent)

    def across(source, target, send, receive, k):
        peer = lax.rem(me + k, experts)
        return pltpu.make_async_remote_copy(
            src_ref=source.at[peer, used],
            dst_ref=target.at[me, used],
            send_sem=send.at[k],
            recv_sem=receive.at[k],
            device_id=(peer, side),
            device_id_type=MESH,
        )

    def go(k):
        return across(outgoing, arrived, go_send, go_recv, k)

    def back(k):
        return across(results, returned, back_send, back_recv, k)

    def forward(k):
        source = lax.rem(me - k + experts, experts)
        return pltpu.make_async_remote_copy(
            src_ref=arrived.at[source, used],
            dst_ref=paired.at[source, used],
            send_sem=fwd_send.at[k],
            recv_sem=fwd_recv.at[k],
            device_id=(me, other),
            device_id_type=MESH,
        )

    def keep(source, target, index):
        return pltpu.make_async_copy(
            source.at[me, used], target.at[me, used], local_sems.at[index]
        )

    @pl.loop(1, experts)
    def _(j):
        go(lax.rem(j + experts // 2 - 2, experts - 1) + 1).start()

    keep(outgoing, arrived, 0).start()
    steps = cells // chunk
    for c in range(steps // 2):
        update_state(c)
    keep(outgoing, arrived, 0).wait()
    forward(0).start()

    @pl.loop(1, experts)
    def _(k):
        go(k).wait_recv()
        forward(k).start()

    x = arrived[...].astype(F32).reshape(places, half).astype(BF16)
    copies[8].wait()
    copies[9].wait()
    gate = dot(x, e_gate[own_part, :])
    up = dot(x, e_up[own_part, :])

    @pl.loop(0, experts)
    def _(k):
        forward(k).wait_recv()

    x = paired[...].astype(F32).reshape(places, half).astype(BF16)
    gate = gate + dot(x, e_gate[other_part, :])
    up = up + dot(x, e_up[other_part, :])
    hidden = (jax.nn.silu(gate) * up).astype(BF16)
    copies[10].wait()
    crossing[...] = dot(hidden, e_down[:, other_part]).astype(BF16)
    cross_copy = to_pair(crossing, crossed, 1)
    cross_copy.start()
    own_result = dot(hidden, e_down[:, own_part])
    cross_copy.wait()
    own_result = own_result + crossed[...].astype(F32)
    results[...] = own_result.reshape(experts, capacity, half).astype(BF16)

    @pl.loop(1, experts)
    def _(j):
        back(lax.rem(j + experts // 2 - 2, experts - 1) + 1).start()

    keep(results, returned, 1).start()
    for c in range(steps // 2, steps):
        update_state(c)
    keep(results, returned, 1).wait()

    @pl.loop(1, experts)
    def _(k):
        back(k).wait_recv()

    y = returned[...].astype(F32).reshape(places, half).astype(BF16)
    turned = (((0,), (0,)), ((), ()))
    total = (
        own_residual
        + weight0 * lax.dot_general(place0, y, turned, preferred_element_type=F32)
        + weight1 * lax.dot_general(place1, y, turned, preferred_element_type=F32)
    )
    final[...] = total.astype(BF16)
    final_copy = to_pair(final, out_ref.at[:, own_part], 2)
    final_copy.start()
    out_ref[:, own_part] = final[...]
    final_copy.wait()

    forward(0).wait_send()

    @pl.loop(1, experts)
    def _(k):
        go(k).wait_send()
        forward(k).wait_send()
        back(k).wait_send()


def store_kernel(layer_ref, state_ref, layer_out, state_out, sems):
    first = pltpu.make_async_copy(state_ref, state_out, sems.at[0])
    second = pltpu.make_async_copy(layer_ref, layer_out, sems.at[1])
    first.start()
    second.start()
    first.wait()
    second.wait()


def body(
    tokens,
    linear_matrix_state,
    mixer_norm_gain,
    receptance_weight,
    key_weight,
    value_weight,
    decay_weight,
    learning_rate_weight,
    output_gate_weight,
    decay_offset_bias,
    present_position_factor,
    per_head_gain,
    head_mix_weight,
    feedforward_gain,
    routing,
    router_score,
    expert_gate_weight,
    expert_up_weight,
    expert_down_weight,
):
    seqs, model = tokens.shape
    _, heads, cells = linear_matrix_state.shape
    rows = seqs * heads
    weights = (
        receptance_weight,
        key_weight,
        value_weight,
        decay_weight,
        learning_rate_weight,
        output_gate_weight,
    )
    experts = lax.axis_size("ep")
    sent = max(2, 8 * seqs * routing.shape[1] // (3 * experts))
    sent = -(-sent // 2) * 2
    capacity = -(-sent // 8) * 8
    half = model // 2
    exchange = pltpu.VMEM((experts, capacity, half), BF16)
    crosswise = pltpu.VMEM((experts * capacity, half), BF16)
    layer, state = pl.pallas_call(
        functools.partial(layer_kernel, experts, capacity, sent),
        out_shape=(
            pltpu.VMEM((seqs, model), BF16),
            pltpu.VMEM(linear_matrix_state.shape, F32),
        ),
        in_specs=[VMEM, HBM, VMEM] + [HBM] * 6 + [VMEM] * 3 + [HBM] + [VMEM] * 3 + [HBM] * 3,
        out_specs=(VMEM, VMEM),
        scratch_shapes=[pltpu.VMEM(w.shape, BF16) for w in weights]
        + [pltpu.VMEM(head_mix_weight.shape, BF16)]
        + [pltpu.VMEM((rows, LANES), F32)] * 8
        + [
            pltpu.VMEM((3 * rows, cells), BF16),
            pltpu.VMEM((cells, LANES), BF16),
            pltpu.VMEM(expert_gate_weight.shape[1:], BF16),
            pltpu.VMEM(expert_up_weight.shape[1:], BF16),
            pltpu.VMEM(expert_down_weight.shape[1:], BF16),
            pltpu.VMEM((seqs, model), BF16),
            pltpu.VMEM((seqs, model), BF16),
            exchange,
            exchange,
            exchange,
            crosswise,
            crosswise,
            exchange,
            exchange,
            pltpu.VMEM((seqs, half), BF16),
            pltpu.SemaphoreType.DMA((11,)),
            pltpu.SemaphoreType.DMA((3,)),
            pltpu.SemaphoreType.DMA((3,)),
        ]
        + [pltpu.SemaphoreType.DMA((experts,))] * 6
        + [pltpu.SemaphoreType.DMA((2,))],
        compiler_params=pltpu.CompilerParams(
            collective_id=0, has_side_effects=True, vmem_limit_bytes=61 * 2**20
        ),
        name="layer",
    )(
        tokens,
        linear_matrix_state,
        mixer_norm_gain.reshape(1, -1),
        *weights,
        decay_offset_bias.reshape(1, -1),
        present_position_factor.reshape(1, -1),
        per_head_gain.reshape(1, -1),
        head_mix_weight,
        feedforward_gain.reshape(1, -1),
        routing.T,
        router_score.T,
        expert_gate_weight,
        expert_up_weight,
        expert_down_weight,
    )
    return pl.pallas_call(
        store_kernel,
        out_shape=(
            jax.ShapeDtypeStruct((seqs, model), BF16),
            jax.ShapeDtypeStruct(linear_matrix_state.shape, F32),
        ),
        in_specs=[VMEM, VMEM],
        out_specs=(HBM, HBM),
        scratch_shapes=[pltpu.SemaphoreType.DMA((2,))],
        compiler_params=pltpu.CompilerParams(vmem_limit_bytes=4 * 2**20),
        name="store",
    )(layer, state)


def solution(mesh):
    return jax.shard_map(
        body,
        mesh=mesh,
        in_specs=(
            P("ep", None),
            P("ep", "tp", None),
            P(),
            P(None, "tp"),
            P(None, "tp"),
            P(None, "tp"),
            P(None, "tp"),
            P(None, "tp"),
            P(None, "tp"),
            P("tp"),
            P("tp"),
            P("tp"),
            P("tp", None),
            P(),
            P("ep", None),
            P("ep", None),
            P("ep", None, "tp"),
            P("ep", None, "tp"),
            P("ep", "tp", None),
        ),
        out_specs=(P("ep", None), P("ep", "tp", None)),
        check_vma=False,
    )
```

```python
import functools
import math

import jax
import jax.numpy as jnp
from jax import lax
from jax.experimental import pallas as pl
from jax.experimental.pallas import tpu as pltpu
from jax.sharding import PartitionSpec as P

NORM_EPS = 1e-06
UNIT_EPS = 1e-05
HEAD_EPS = 0.00064
LANES = 128
F32 = jnp.float32
BF16 = jnp.bfloat16
HBM = pl.BlockSpec(memory_space=pl.ANY)
VMEM = pl.BlockSpec(memory_space=pltpu.VMEM)
MESH = pl.DeviceIdType.MESH
DECAY_SCALE = math.exp(-0.5)


def dot(a, b):
    return jnp.dot(a, b, preferred_element_type=F32)


def rms_scale(values, gain):
    factor = lax.rsqrt(jnp.mean(values * values, axis=-1, keepdims=True) + NORM_EPS)
    return values * factor * gain


def split(x):
    high = x.astype(BF16)
    return high, (x - high.astype(F32)).astype(BF16)


def to_head_rows(x, ref, heads):
    seqs = x.shape[0]
    low = lax.broadcasted_iota(jnp.int32, (seqs, LANES), 1) < LANES // 2
    for pair in range(heads // 2):
        here = x[:, pair * LANES : (pair + 1) * LANES]
        turned = pltpu.roll(here, LANES // 2, 1)
        ref[pl.ds(2 * pair, seqs, stride=heads), :] = jnp.where(low, here, turned)
        ref[pl.ds(2 * pair + 1, seqs, stride=heads), :] = jnp.where(low, turned, here)


def from_head_rows(ref, seqs, heads):
    low = lax.broadcasted_iota(jnp.int32, (seqs, LANES), 1) < LANES // 2
    parts = []
    for pair in range(heads // 2):
        even = ref[pl.ds(2 * pair, seqs, stride=heads), :]
        odd = ref[pl.ds(2 * pair + 1, seqs, stride=heads), :]
        parts.append(jnp.where(low, even, odd))
    return jnp.concatenate(parts, axis=1)


def layer_kernel(
    experts,
    capacity,
    sent,
    tokens_ref,
    state_hbm,
    norm_gain_ref,
    wr_hbm,
    wk_hbm,
    wv_hbm,
    wd_hbm,
    wl_hbm,
    wg_hbm,
    bias_ref,
    factor_ref,
    head_gain_ref,
    wm_hbm,
    gain_ref,
    routing_ref,
    score_ref,
    gate_hbm,
    up_hbm,
    down_hbm,
    out_ref,
    state,
    wr,
    wk,
    wv,
    wd,
    wl,
    wg,
    wm,
    r_rows,
    k_rows,
    v_rows,
    d_rows,
    l_rows,
    f_rows,
    g_rows,
    o_rows,
    products,
    gatherer,
    e_gate,
    e_up,
    e_down,
    own_partial,
    other_partial,
    outgoing,
    arrived,
    paired,
    crossing,
    crossed,
    results,
    returned,
    final,
    sems,
    pair_send,
    pair_recv,
    go_send,
    go_recv,
    fwd_send,
    fwd_recv,
    back_send,
    back_recv,
    local_sems,
):
    me = lax.axis_index("ep")
    side = lax.axis_index("tp")
    other = 1 - side
    seqs, heads, cells = state.shape
    rows = seqs * heads
    width = LANES // 2
    model = tokens_ref.shape[1]
    half = model // 2
    places = experts * capacity

    sources = [wk_hbm, wr_hbm, wd_hbm, wl_hbm, state_hbm, wv_hbm, wg_hbm, wm_hbm]
    targets = [wk, wr, wd, wl, state, wv, wg, wm]
    sources += [gate_hbm.at[0], up_hbm.at[0], down_hbm.at[0]]
    targets += [e_gate, e_up, e_down]
    copies = [
        pltpu.make_async_copy(a, b, sems.at[i]) for i, (a, b) in enumerate(zip(sources, targets))
    ]
    for copy in copies:
        copy.start()

    blank = jnp.zeros(arrived.shape, BF16)
    arrived[...] = blank
    paired[...] = blank
    returned[...] = blank

    barrier = pltpu.get_barrier_semaphore()
    pl.semaphore_signal(barrier, inc=1, device_id=(me, other), device_id_type=MESH)

    @pl.loop(1, experts)
    def _(k):
        pl.semaphore_signal(
            barrier, inc=1, device_id=(lax.rem(me + k, experts), side), device_id_type=MESH
        )

    normed = rms_scale(tokens_ref[...].astype(F32), norm_gain_ref[...]).astype(BF16)
    channels = heads * width
    to_head_rows(jnp.broadcast_to(factor_ref[...], (seqs, channels)), f_rows, heads)
    to_head_rows(jnp.broadcast_to(head_gain_ref[...], (seqs, channels)), g_rows, heads)
    chunk = 512
    for c in range(cells // chunk):
        at = lax.broadcasted_iota(jnp.int32, (chunk, LANES), 0) // width
        to = lax.broadcasted_iota(jnp.int32, (chunk, LANES), 1) % width
        gatherer[pl.ds(c * chunk, chunk), :] = jnp.where(
            to - at == c * (chunk // width), 1.0, 0.0
        ).astype(BF16)

    route0 = routing_ref[0:1, :]
    route1 = routing_ref[1:2, :]
    names = lax.broadcasted_iota(jnp.int32, (experts, seqs), 0)
    hot0 = jnp.where(route0 == names, 1.0, 0.0)
    hot1 = jnp.where(route1 == names, 1.0, 0.0)
    row = lax.broadcasted_iota(jnp.int32, (seqs, seqs), 0)
    column = lax.broadcasted_iota(jnp.int32, (seqs, seqs), 1)
    above = jnp.where(row < column, 1.0, 0.0).astype(BF16)
    before0 = dot(hot0.astype(BF16), above)
    before1 = dot(hot1.astype(BF16), above) + jnp.sum(hot0, axis=1, keepdims=True)
    slot0 = jnp.sum(before0 * hot0, axis=0, keepdims=True).astype(jnp.int32)
    slot1 = jnp.sum(before1 * hot1, axis=0, keepdims=True).astype(jnp.int32)
    spots = lax.broadcasted_iota(jnp.int32, (places, seqs), 0)
    place0 = jnp.where(route0 * capacity + slot0 == spots, 1.0, 0.0)
    place1 = jnp.where(route1 * capacity + slot1 == spots, 1.0, 0.0)
    placed = (place0 + place1).astype(BF16)
    place0 = place0.astype(BF16)
    place1 = place1.astype(BF16)
    difference = score_ref[0:1, :] - score_ref[1:2, :]
    difference = jnp.sum(jnp.where(row == column, difference, 0.0), axis=1, keepdims=True)
    weight0 = jax.nn.sigmoid(difference)
    weight1 = jax.nn.sigmoid(-difference)

    for copy in copies[:4]:
        copy.wait()
    to_head_rows(dot(normed, wk[...]), k_rows, heads)
    to_head_rows(dot(normed, wr[...]), r_rows, heads)
    decay_in = dot(normed, wd[...]) + bias_ref[...]
    to_head_rows(jnp.exp(-DECAY_SCALE * jax.nn.sigmoid(decay_in)), d_rows, heads)
    to_head_rows(jax.nn.sigmoid(dot(normed, wl[...])), l_rows, heads)

    key = k_rows[...]
    unit = key * lax.rsqrt(jnp.sum(key * key, axis=-1, keepdims=True) * 0.5 + UNIT_EPS)
    decay = d_rows[...]
    rate = l_rows[...]
    receptance = r_rows[...]
    shifted = key * rate
    unit_rate = unit * rate
    decay_receptance = decay * receptance

    for copy in copies[4:8]:
        copy.wait()
    for c in range(cells // LANES):
        lanes = pl.ds(c * LANES, LANES)
        x = state[:, :, lanes].reshape(rows, LANES)
        products[0:rows, lanes] = (x * unit).astype(BF16)
        high, low = split(x * decay_receptance)
        products[rows : 2 * rows, lanes] = high
        products[2 * rows : 3 * rows, lanes] = low
    to_head_rows(dot(normed, wv[...]), v_rows, heads)
    value = v_rows[...]
    sums = dot(products[...], gatherer[...])
    removed = sums[0:rows]
    read = sums[rows : 2 * rows] + sums[2 * rows :]

    def head_sum(x):
        return jnp.sum(x, axis=-1, keepdims=True) * 0.5

    read = read - removed * head_sum(unit_rate * receptance) + value * head_sum(shifted * receptance)
    center = read - head_sum(read) * (1.0 / width)
    scaled = center * lax.rsqrt(head_sum(center * center) * (1.0 / width) + HEAD_EPS)
    own = head_sum(receptance * shifted * f_rows[...])
    o_rows[...] = scaled * g_rows[...] + own * value
    gating = jax.nn.sigmoid(dot(normed, wg[...]))
    merged = (from_head_rows(o_rows, seqs, heads) * gating).astype(BF16)
    own_partial[...] = dot(merged, wm[...]).astype(BF16)
    pl.semaphore_wait(barrier, experts)

    def to_pair(source, target, index):
        return pltpu.make_async_remote_copy(
            src_ref=source,
            dst_ref=target,
            send_sem=pair_send.at[index],
            recv_sem=pair_recv.at[index],
            device_id=(me, other),
            device_id_type=MESH,
        )

    mix_copy = to_pair(own_partial, other_partial, 0)
    mix_copy.start()
    first = lax.broadcasted_iota(jnp.int32, (rows, LANES), 1) < width
    v_high, v_low = split(value)
    m_high, m_low = split(removed)
    compact = jnp.concatenate(
        [
            jnp.where(first, v_high.astype(F32), v_low.astype(F32)).astype(BF16),
            jnp.where(first, m_high.astype(F32), m_low.astype(F32)).astype(BF16),
        ],
        axis=0,
    )

    def update_state(c):
        spread = lax.dot_general(
            compact,
            gatherer[pl.ds(c * chunk, chunk), :],
            (((1,), (1,)), ((), ())),
            preferred_element_type=F32,
        )
        for b in range(chunk // LANES):
            lanes = pl.ds(c * chunk + b * LANES, LANES)
            x = state[:, :, lanes].reshape(rows, LANES)
            v_here = spread[0:rows, b * LANES : (b + 1) * LANES]
            m_here = spread[rows:, b * LANES : (b + 1) * LANES]
            new = x * decay + v_here * shifted - m_here * unit_rate
            state[:, :, lanes] = new.reshape(seqs, heads, LANES)

    mix_copy.wait()
    mix = (own_partial[...].astype(F32) + other_partial[...].astype(F32)).astype(BF16)
    residual = tokens_ref[...].astype(F32) + mix.astype(F32)
    expert_in = rms_scale(residual, gain_ref[...])
    own_part = pl.ds(pl.multiple_of(side * half, LANES), half)
    other_part = pl.ds(pl.multiple_of(other * half, LANES), half)
    mine = jnp.where(side == 0, expert_in[:, :half], expert_in[:, half:]).astype(BF16)
    own_residual = jnp.where(side == 0, residual[:, :half], residual[:, half:])
    outgoing[...] = dot(placed, mine).reshape(experts, capacity, half).astype(BF16)
    used = pl.ds(0, sent)

    def across(source, target, send, receive, k):
        peer = lax.rem(me + k, experts)
        return pltpu.make_async_remote_copy(
            src_ref=source.at[peer, used],
            dst_ref=target.at[me, used],
            send_sem=send.at[k],
            recv_sem=receive.at[k],
            device_id=(peer, side),
            device_id_type=MESH,
        )

    def go(k):
        return across(outgoing, arrived, go_send, go_recv, k)

    def back(k):
        return across(results, returned, back_send, back_recv, k)

    def forward(k):
        source = lax.rem(me - k + experts, experts)
        return pltpu.make_async_remote_copy(
            src_ref=arrived.at[source, used],
            dst_ref=paired.at[source, used],
            send_sem=fwd_send.at[k],
            recv_sem=fwd_recv.at[k],
            device_id=(me, other),
            device_id_type=MESH,
        )

    def keep(source, target, index):
        return pltpu.make_async_copy(
            source.at[me, used], target.at[me, used], local_sems.at[index]
        )

    @pl.loop(1, experts)
    def _(j):
        go(lax.rem(j + experts // 2 - 2, experts - 1) + 1).start()

    keep(outgoing, arrived, 0).start()
    steps = cells // chunk
    for c in range(steps // 2):
        update_state(c)
    keep(outgoing, arrived, 0).wait()
    forward(0).start()

    @pl.loop(1, experts)
    def _(k):
        go(k).wait_recv()
        forward(k).start()

    x = arrived[...].astype(F32).reshape(places, half).astype(BF16)
    copies[8].wait()
    copies[9].wait()
    gate = dot(x, e_gate[own_part, :])
    up = dot(x, e_up[own_part, :])

    @pl.loop(0, experts)
    def _(k):
        forward(k).wait_recv()

    x = paired[...].astype(F32).reshape(places, half).astype(BF16)
    gate = gate + dot(x, e_gate[other_part, :])
    up = up + dot(x, e_up[other_part, :])
    hidden = (jax.nn.silu(gate) * up).astype(BF16)
    copies[10].wait()
    crossing[...] = dot(hidden, e_down[:, other_part]).astype(BF16)
    cross_copy = to_pair(crossing, crossed, 1)
    cross_copy.start()
    own_result = dot(hidden, e_down[:, own_part])
    cross_copy.wait()
    own_result = own_result + crossed[...].astype(F32)
    results[...] = own_result.reshape(experts, capacity, half).astype(BF16)

    @pl.loop(1, experts)
    def _(j):
        back(lax.rem(j + experts // 2 - 2, experts - 1) + 1).start()

    keep(results, returned, 1).start()
    for c in range(steps // 2, steps):
        update_state(c)
    keep(results, returned, 1).wait()

    @pl.loop(1, experts)
    def _(k):
        back(k).wait_recv()

    y = returned[...].astype(F32).reshape(places, half).astype(BF16)
    turned = (((0,), (0,)), ((), ()))
    total = (
        own_residual
        + weight0 * lax.dot_general(place0, y, turned, preferred_element_type=F32)
        + weight1 * lax.dot_general(place1, y, turned, preferred_element_type=F32)
    )
    final[...] = total.astype(BF16)
    final_copy = to_pair(final, out_ref.at[:, own_part], 2)
    final_copy.start()
    out_ref[:, own_part] = final[...]
    final_copy.wait()

    forward(0).wait_send()

    @pl.loop(1, experts)
    def _(k):
        go(k).wait_send()
        forward(k).wait_send()
        back(k).wait_send()


def store_kernel(layer_ref, state_ref, layer_out, state_out, sems):
    first = pltpu.make_async_copy(state_ref, state_out, sems.at[0])
    second = pltpu.make_async_copy(layer_ref, layer_out, sems.at[1])
    first.start()
    second.start()
    first.wait()
    second.wait()


def body(
    tokens,
    linear_matrix_state,
    mixer_norm_gain,
    receptance_weight,
    key_weight,
    value_weight,
    decay_weight,
    learning_rate_weight,
    output_gate_weight,
    decay_offset_bias,
    present_position_factor,
    per_head_gain,
    head_mix_weight,
    feedforward_gain,
    routing,
    router_score,
    expert_gate_weight,
    expert_up_weight,
    expert_down_weight,
):
    seqs, model = tokens.shape
    _, heads, cells = linear_matrix_state.shape
    rows = seqs * heads
    weights = (
        receptance_weight,
        key_weight,
        value_weight,
        decay_weight,
        learning_rate_weight,
        output_gate_weight,
    )
    experts = lax.axis_size("ep")
    sent = max(2, 8 * seqs * routing.shape[1] // (3 * experts))
    sent = -(-sent // 2) * 2
    capacity = -(-sent // 8) * 8
    half = model // 2
    exchange = pltpu.VMEM((experts, capacity, half), BF16)
    crosswise = pltpu.VMEM((experts * capacity, half), BF16)
    layer, state = pl.pallas_call(
        functools.partial(layer_kernel, experts, capacity, sent),
        out_shape=(
            pltpu.VMEM((seqs, model), BF16),
            pltpu.VMEM(linear_matrix_state.shape, F32),
        ),
        in_specs=[VMEM, HBM, VMEM] + [HBM] * 6 + [VMEM] * 3 + [HBM] + [VMEM] * 3 + [HBM] * 3,
        out_specs=(VMEM, VMEM),
        scratch_shapes=[pltpu.VMEM(w.shape, BF16) for w in weights]
        + [pltpu.VMEM(head_mix_weight.shape, BF16)]
        + [pltpu.VMEM((rows, LANES), F32)] * 8
        + [
            pltpu.VMEM((3 * rows, cells), BF16),
            pltpu.VMEM((cells, LANES), BF16),
            pltpu.VMEM(expert_gate_weight.shape[1:], BF16),
            pltpu.VMEM(expert_up_weight.shape[1:], BF16),
            pltpu.VMEM(expert_down_weight.shape[1:], BF16),
            pltpu.VMEM((seqs, model), BF16),
            pltpu.VMEM((seqs, model), BF16),
            exchange,
            exchange,
            exchange,
            crosswise,
            crosswise,
            exchange,
            exchange,
            pltpu.VMEM((seqs, half), BF16),
            pltpu.SemaphoreType.DMA((11,)),
            pltpu.SemaphoreType.DMA((3,)),
            pltpu.SemaphoreType.DMA((3,)),
        ]
        + [pltpu.SemaphoreType.DMA((experts,))] * 6
        + [pltpu.SemaphoreType.DMA((2,))],
        compiler_params=pltpu.CompilerParams(
            collective_id=0, has_side_effects=True, vmem_limit_bytes=61 * 2**20
        ),
        name="layer",
    )(
        tokens,
        linear_matrix_state,
        mixer_norm_gain.reshape(1, -1),
        *weights,
        decay_offset_bias.reshape(1, -1),
        present_position_factor.reshape(1, -1),
        per_head_gain.reshape(1, -1),
        head_mix_weight,
        feedforward_gain.reshape(1, -1),
        routing.T,
        router_score.T,
        expert_gate_weight,
        expert_up_weight,
        expert_down_weight,
    )
    return pl.pallas_call(
        store_kernel,
        out_shape=(
            jax.ShapeDtypeStruct((seqs, model), BF16),
            jax.ShapeDtypeStruct(linear_matrix_state.shape, F32),
        ),
        in_specs=[VMEM, VMEM],
        out_specs=(HBM, HBM),
        scratch_shapes=[pltpu.SemaphoreType.DMA((2,))],
        compiler_params=pltpu.CompilerParams(vmem_limit_bytes=4 * 2**20),
        name="store",
    )(layer, state)


def solution(mesh):
    return jax.shard_map(
        body,
        mesh=mesh,
        in_specs=(
            P("ep", None),
            P("ep", "tp", None),
            P(),
            P(None, "tp"),
            P(None, "tp"),
            P(None, "tp"),
            P(None, "tp"),
            P(None, "tp"),
            P(None, "tp"),
            P("tp"),
            P("tp"),
            P("tp"),
            P("tp", None),
            P(),
            P("ep", None),
            P("ep", None),
            P("ep", None, "tp"),
            P("ep", None, "tp"),
            P("ep", "tp", None),
        ),
        out_specs=(P("ep", None), P("ep", "tp", None)),
        check_vma=False,
    )
```
